32 devices in a mesh: ep: 32 (over z, y, x, core).
Axes of the slice: x: 2, y: 2, z: 4, core: 2. Of those that a mesh axis runs over, the one named last changes fastest.
Arguments:
- tokens: bfloat16 [640, 2048], P('ep'), may hold values from -6 to 6
- positions: int32 [640], P('ep'), may hold values from 1024 to 16383
- state: float32 [640, 8, 64, 128], P('ep'), may hold values from -1.6 to 1.6
- mix_gain: float32 [2048], replicated, may hold values from 0.1 to 1.9
- w_query: bfloat16 [2048, 512], replicated, may hold values from -0.125 to 0.125
- w_key: bfloat16 [2048, 512], replicated, may hold values from -0.125 to 0.125
- w_value: bfloat16 [2048, 1024], replicated, may hold values from -0.125 to 0.125
- ret_gain: float32 [1024], replicated, may hold values from 0.1 to 1.9
- w_out: bfloat16 [1024, 2048], P(None, 'ep'), may hold values from -0.1875 to 0.1875
- ffn_gain: float32 [2048], replicated, may hold values from 0.1 to 1.9
- routes: int32 [640, 6], P('ep'), may hold values from 0 to 31, all different within a row; in each aligned block of 20 rows (0 to 19, 20 to 39, ...) at most 7 rows name the same one
- route_weights: float32 [640, 6], P('ep'), may hold values from 0.1 to 1
- expert_gate: bfloat16 [32, 2048, 512], P('ep'), may hold values from -0.125 to 0.125
- expert_up: bfloat16 [32, 2048, 512], P('ep'), may hold values from -0.125 to 0.125
- expert_down: bfloat16 [32, 512, 2048], P('ep'), may hold values from -0.25 to 0.25
Outputs:
- result: bfloat16 [640, 2048], P('ep')
- new_state: float32 [640, 8, 64, 128], P('ep')
The draws below stay inside these ranges and needn't reach their ends.
Inputs may be any that keep to these rules, and one draw needn't show every extreme that they name: `routes`: each row names 6 different experts; among the rows of one device no expert is named more than 7 times, a bound that some block reaches there.
All inputs are finite; a program needn't handle non-finite values.
Results may differ from the reference program's by a relative error of at most 0.017.
Values may be sent and summed in bfloat16 or wider, within the bound.
No kernel may reach another device: no remote copies, remote signals or barrier semaphores. Data moves between devices by JAX's collectives and lax.ppermute only.
A program may use at most 128 MiB of HBM per device.

```python
import math
import jax
import jax.numpy as jnp
import numpy as np
from jax import lax

D = 2048
HEADS = 8
HEAD_K = 64
HEAD_V = 128
FE = 512
TOPK = 6
SEQ_DEV = 20
QK = 512
VW = 1024
EXPERTS = 32
CAP = 7
TOKENS = 640
N_EP = 32


def touch_ends(values, own_key, smallest, top_value):
    longest = values.shape.index(max(values.shape))
    spots = []
    for shift in (0, 1):
        where = [jax.random.randint(jax.random.fold_in(own_key, axis), (), 0, length) for axis, length in enumerate(values.shape)]
        where[longest] = (where[longest] + shift) % values.shape[longest]
        spots.append(tuple(where))
    return values.at[spots[0]].set(smallest).at[spots[1]].set(top_value)


def shard_levels(rng, extent, pieces, smallest, high):
    level = 1.0
    for dim, blocks in pieces:
        heights = jax.random.uniform(jax.random.fold_in(jax.random.fold_in(rng, 6), dim), (blocks,), jnp.float32, smallest / len(pieces), high / len(pieces))
        level = level * jnp.repeat(jnp.exp(heights), extent[dim] // blocks).reshape((-1,) + (1,) * (len(extent) - 1 - dim))
    return level


def assign_block(stream_key, own, number, rows, count, top, bound, skew):
    order = jax.random.permutation(stream_key, count)
    crowded, common = portions_of(count, rows * top, bound, skew, True), portions_of(count, rows * top, bound, skew, False)
    places = jnp.arange(count)

    def named(sizes, rotation):
        used = int((sizes > 0).sum())
        fixed = max(1, used // 4)
        passed = fixed + (places - fixed + rotation * (used - fixed)) % max(1, count - fixed)
        return jnp.zeros((count,), jnp.int32).at[order[jnp.where(places < fixed, places, passed)]].set(jnp.asarray(sizes, jnp.int32))

    sizes = jnp.where(number % 4 == 0, named(crowded, number // 4), named(common, number - number // 4 - 1))
    mixed = jax.random.permutation(jax.random.fold_in(own, 3), count)
    donor, receiver = mixed[0:count // 2 * 2:2], mixed[1:count // 2 * 2:2]
    margin = jnp.minimum(sizes[donor] - 1, bound - sizes[receiver]) // 2
    margin = jnp.where((donor == order[0]) | (receiver == order[0]) | (sizes[receiver] == 0), 0, jnp.maximum(margin, 0))
    passed = jax.random.randint(jax.random.fold_in(own, 4), (count // 2,), 0, 1 << 20) % (margin + 1)
    sizes = sizes.at[donor].add(-passed).at[receiver].add(passed)
    items = jnp.searchsorted(jnp.cumsum(sizes), jnp.arange(rows * top), side="right").astype(jnp.int32)
    listing = items.reshape(top, rows).T
    listing = listing[jax.random.permutation(jax.random.fold_in(own, 1), rows)]
    rotation = jax.random.randint(jax.random.fold_in(own, 2), (rows, 1), 0, top)
    return jnp.take_along_axis(listing, (jnp.arange(top)[None, :] + rotation) % top, axis=1)


def portions_of(amount, total, limit, lean, full):
    weights = [(1 << 20) // math.isqrt(standing ** lean) + 1 for standing in range(1, amount + 1)]
    largest = limit if full else min(limit, max(-(-total // amount), total * weights[0] // sum(weights)))
    least = 1 if total - largest >= amount - 1 else 0
    given, spare = [largest] + [least] * (amount - 1), total - largest - least * (amount - 1)
    while spare > 0:
        free = [i for i in range(1, amount) if given[i] < largest] or [i for i in range(1, amount) if given[i] < limit]
        mass, remaining = sum([weights[i] for i in free]), spare
        for i in free:
            extra = min(limit - given[i], max(1, remaining * weights[i] // mass), spare)
            given[i] = given[i] + extra
            spare = spare - extra
    return np.array(given)


def bell_draw(key, shape, spread, reach, cuts=(), held_as=jnp.bfloat16):
    values = jax.random.normal(key, shape, jnp.float32) * spread
    if len(cuts) > 0:
        values = shard_levels(key, shape, cuts, -0.22, 0.18) * values
    return jnp.clip(values, min=-reach, max=reach).astype(held_as)


def setup_inputs(seed: int = 0) -> dict:
    key_list = jax.random.split(jax.random.key(seed), 16)
    tokens = bell_draw(key_list[0], (TOKENS, D), 1.0, 6.0, ((0, 32),))
    positions = touch_ends(jax.random.randint(key_list[1], (TOKENS,), 1024, 16384), jax.random.fold_in(key_list[1], 1), 1024, 16383).astype(jnp.int32)
    state = bell_draw(key_list[2], (TOKENS, HEADS, HEAD_K, HEAD_V), 0.2, 1.6, ((0, 32),), jnp.float32)
    mix_gain = jnp.clip(1.0 + 0.18 * jax.random.normal(key_list[3], (D,), jnp.float32), 0.1, 1.9)
    w_query = bell_draw(key_list[4], (D, QK), D ** -0.5, 0.125)
    w_key = bell_draw(key_list[5], (D, QK), D ** -0.5, 0.125)
    w_value = bell_draw(key_list[6], (D, VW), D ** -0.5, 0.125)
    ret_gain = jnp.clip(1.0 + 0.18 * jax.random.normal(key_list[7], (VW,), jnp.float32), 0.1, 1.9)
    w_out = bell_draw(key_list[8], (VW, D), VW ** -0.5, 0.1875, ((1, 32),))
    ffn_gain = jnp.clip(1.0 + 0.18 * jax.random.normal(key_list[9], (D,), jnp.float32), 0.1, 1.9)
    routes_keys = jax.random.split(jax.random.fold_in(key_list[10], 1), TOKENS // SEQ_DEV)
    routes_turns = jax.random.permutation(jax.random.fold_in(key_list[10], 3), TOKENS // SEQ_DEV)
    routes = jax.vmap(lambda own, number: assign_block(jax.random.fold_in(key_list[10], 2), own, number, SEQ_DEV, EXPERTS, TOPK, CAP, 1))(routes_keys, routes_turns).reshape((TOKENS, TOPK))
    route_weights = jnp.clip(0.1 + 0.9 * jax.random.uniform(key_list[11], (TOKENS, TOPK), jnp.float32) ** shard_levels(key_list[11], (TOKENS, TOPK), ((0, 32),), -0.2, 0.2), 0.1, 1.0)
    expert_gate = bell_draw(key_list[12], (EXPERTS, D, FE), D ** -0.5, 0.125, ((0, 32),))
    expert_up = bell_draw(key_list[13], (EXPERTS, D, FE), D ** -0.5, 0.125, ((0, 32),))
    expert_down = bell_draw(key_list[14], (EXPERTS, FE, D), FE ** -0.5, 0.25, ((0, 32),))
    return {"tokens": tokens, "positions": positions, "state": state, "mix_gain": mix_gain, "w_query": w_query, "w_key": w_key, "w_value": w_value, "ret_gain": ret_gain, "w_out": w_out, "ffn_gain": ffn_gain, "routes": routes, "route_weights": route_weights, "expert_gate": expert_gate, "expert_up": expert_up, "expert_down": expert_down}


EPS = 1e-06

def rms_scale(values, gain):
    wide = values.astype(jnp.float32)
    scaled = wide * lax.rsqrt(lax.optimization_barrier(jnp.mean(wide * wide, axis=-1, keepdims=True)) + EPS)
    return (scaled * gain.astype(jnp.float32)).astype(jnp.bfloat16)

def rotate(field, spots):
    half = field.shape[-1] // 2
    freqs = jnp.exp(-math.log(10000.0) * jnp.arange(half, dtype=jnp.float32) / half)
    angle = spots.astype(jnp.float32)[:, None] * freqs[None, :]
    cosine = jnp.cos(angle)[:, None, :]
    sine = jnp.sin(angle)[:, None, :]
    first = field[..., :half]
    second = field[..., half:]
    return jnp.concatenate([first * cosine - second * sine, second * cosine + first * sine], axis=-1)

def reference(tokens, positions, state, mix_gain, w_query, w_key, w_value, ret_gain, w_out, ffn_gain, routes, route_weights, expert_gate, expert_up, expert_down):
    normed_in = rms_scale(tokens, mix_gain)
    q_proj = jnp.dot(normed_in, w_query, preferred_element_type=jnp.float32).astype(jnp.bfloat16)
    k_proj = jnp.dot(normed_in, w_key, preferred_element_type=jnp.float32).astype(jnp.bfloat16)
    v_proj = jnp.dot(normed_in, w_value, preferred_element_type=jnp.float32).astype(jnp.bfloat16)
    queries = rotate(q_proj.astype(jnp.float32).reshape(TOKENS, HEADS, HEAD_K), positions)
    key_rows = rotate(k_proj.astype(jnp.float32).reshape(TOKENS, HEADS, HEAD_K), positions) * HEAD_K ** (-0.5)
    values = v_proj.astype(jnp.float32).reshape(TOKENS, HEADS, HEAD_V)
    decays = 1.0 - jnp.exp2(-2.0 - jnp.arange(HEADS, dtype=jnp.float32))
    new_state = decays[None, :, None, None] * state + key_rows[:, :, :, None] * values[:, :, None, :]
    readout = jnp.einsum('thd,thdv->thv', queries, new_state, precision=lax.Precision.HIGHEST)
    centre = lax.optimization_barrier(jnp.mean(readout, axis=-1, keepdims=True))
    variance = lax.optimization_barrier(jnp.mean(jnp.square(readout - centre), axis=-1, keepdims=True))
    normed = ((readout - centre) * lax.rsqrt(variance + EPS)).reshape(TOKENS, VW) * ret_gain
    mixed = normed.astype(jnp.bfloat16)
    attended = jnp.dot(mixed, w_out, preferred_element_type=jnp.float32).astype(jnp.bfloat16)
    resid = (tokens.astype(jnp.float32) + attended.astype(jnp.float32)).astype(jnp.bfloat16)
    normed_mid = rms_scale(resid, ffn_gain)
    per_dev = SEQ_DEV * TOPK
    chosen = routes.reshape(N_EP, per_dev).astype(jnp.int32)
    matches = (chosen[:, :, None] == jnp.arange(EXPERTS, dtype=jnp.int32)[None, None, :]).astype(jnp.int32)
    places = lax.optimization_barrier(jnp.sum((jnp.cumsum(matches, axis=1) - matches) * matches, axis=-1))
    dev_ids = jnp.arange(N_EP, dtype=jnp.int32)[:, None]
    targets = (chosen * (N_EP * CAP) + dev_ids * CAP + places).reshape(-1).astype(jnp.int32)
    row_ids = jnp.arange(TOKENS * TOPK, dtype=jnp.int32)
    table = jnp.full((EXPERTS * N_EP * CAP,), -1, jnp.int32).at[targets].set(row_ids)
    table = table.reshape(EXPERTS, N_EP * CAP)

    def serve(items):
        gate_w, up_w, down_w, ids = items
        picked = jnp.where(ids[:, None] >= 0, normed_mid[jnp.maximum(ids, 0) // TOPK], jnp.zeros((), jnp.bfloat16))
        picked = picked.astype(jnp.bfloat16)
        gate_part = jnp.dot(picked, gate_w, preferred_element_type=jnp.float32)
        up_part = jnp.dot(picked, up_w, preferred_element_type=jnp.float32)
        hidden = (jax.nn.silu(gate_part) * up_part).astype(jnp.bfloat16)
        return jnp.dot(hidden, down_w, preferred_element_type=jnp.float32).astype(jnp.bfloat16)
    outputs = lax.map(serve, (expert_gate, expert_up, expert_down, table))
    picked_rows = outputs.reshape(-1, D)[targets].astype(jnp.float32)
    mixture = lax.optimization_barrier(jnp.sum(picked_rows.reshape(TOKENS, TOPK, D) * route_weights[:, :, None], axis=1))
    result = (resid.astype(jnp.float32) + mixture).astype(jnp.bfloat16)
    return (result, new_state)
```

```python
import math

import jax
import jax.numpy as jnp
from jax import lax
from jax.sharding import PartitionSpec as P

EPS = 1e-06


def rms_scale(values, gain):
    wide = values.astype(jnp.float32)
    scaled = wide * lax.rsqrt(jnp.mean(wide * wide, axis=-1, keepdims=True) + EPS)
    return (scaled * gain).astype(jnp.bfloat16)


def rotate(field, spots):
    half = field.shape[-1] // 2
    freqs = jnp.exp(-math.log(10000.0) * jnp.arange(half, dtype=jnp.float32) / half)
    angle = spots.astype(jnp.float32)[:, None] * freqs[None, :]
    cosine = jnp.cos(angle)[:, None, :]
    sine = jnp.sin(angle)[:, None, :]
    first = field[..., :half]
    second = field[..., half:]
    return jnp.concatenate(
        [first * cosine - second * sine, second * cosine + first * sine], axis=-1
    )


def in_order(pieces, turn):
    count = len(pieces)
    ordered = []
    for spot in range(count):
        chosen = pieces[0]
        for s in range(1, count):
            chosen = jnp.where((turn - spot) % count == s, pieces[s], chosen)
        ordered.append(chosen)
    return ordered


def share_tokens(tokens, routes, route_weights, plane, planes, group, total):
    width = tokens.shape[1]
    topk = routes.shape[1]
    high = route_weights.astype(jnp.bfloat16)
    low = (route_weights - high.astype(jnp.float32)).astype(jnp.bfloat16)
    extra = jnp.concatenate(
        [(routes // 256).astype(jnp.bfloat16), (routes % 256).astype(jnp.bfloat16), high, low],
        axis=1,
    )
    extra = jnp.pad(extra, ((0, 0), (0, -extra.shape[1] % 128)))
    packed = jnp.concatenate([tokens, extra], axis=1)
    pieces = [packed] + [
        lax.ppermute(packed, "ep", [(d, (d + s * group) % total) for d in range(total)])
        for s in range(1, planes)
    ]
    gathered = jnp.concatenate(in_order(pieces, plane), axis=0)
    small = gathered[:, width:].astype(jnp.float32)
    chosen = (small[:, :topk] * 256.0 + small[:, topk : 2 * topk]).astype(jnp.int32)
    halves = (small[:, 2 * topk : 3 * topk], small[:, 3 * topk : 4 * topk])
    return gathered[:, :width], chosen, halves


def plan(chosen, halves, plane, place, planes, group, seqs, slots):
    rows = chosen.shape[0]
    local = plane * group + (place ^ jnp.arange(group, dtype=jnp.int32))
    match = chosen[:, :, None] == local[None, None, :]
    hit = jnp.any(match, axis=1)
    high, low = (jnp.sum(jnp.where(match, half[:, :, None], 0.0), axis=1) for half in halves)
    before = jnp.arange(rows)[:, None] > jnp.arange(rows)[None, :]
    spot = jnp.dot(
        before.astype(jnp.bfloat16), hit.astype(jnp.bfloat16), preferred_element_type=jnp.float32
    ).astype(jnp.int32)
    spot = jnp.where(hit, spot, -1)
    one_hot = spot[:, :, None] == jnp.arange(slots, dtype=jnp.int32)[None, None, :]
    dispatch = jnp.transpose(one_hot, (1, 2, 0)).reshape(group * slots, rows).astype(jnp.bfloat16)
    combine = [
        jnp.where(one_hot, half[:, :, None], 0.0)
        .astype(jnp.bfloat16)
        .reshape(planes, seqs, group * slots)
        for half in (high, low)
    ]
    return dispatch, jnp.stack(combine, axis=1)


def share_columns(w_out, place, group, total):
    mine = w_out.T
    each = mine.shape[0]
    gathered = jnp.zeros((group * each, mine.shape[1]), mine.dtype)
    for s in range(group):
        piece = mine if s == 0 else lax.ppermute(mine, "ep", [(d, d ^ s) for d in range(total)])
        gathered = lax.dynamic_update_slice_in_dim(gathered, piece, (place ^ s) * each, 0)
    return gathered


def shards(
    tokens,
    positions,
    state,
    mix_gain,
    w_query,
    w_key,
    w_value,
    ret_gain,
    w_out,
    ffn_gain,
    routes,
    route_weights,
    expert_gate,
    expert_up,
    expert_down,
):
    seqs = tokens.shape[0]
    width = tokens.shape[1]
    heads = state.shape[1]
    head_k = state.shape[2]
    head_v = state.shape[3]
    total = lax.axis_size("ep")
    planes = 2 ** ((total.bit_length() - 1) // 2)
    group = total // planes
    index = lax.axis_index("ep")
    plane = index // group
    place = index % group
    topk = routes.shape[1]
    row_count = seqs * topk
    held = expert_gate.shape[0]
    experts = held * total
    capacity = max(2, 2 * row_count // experts) * planes
    slots = -(-capacity // 16) * 16
    tokens_all, routes_all, weights_all = share_tokens(
        tokens, routes, route_weights, plane, planes, group, total
    )
    dispatch, combine = plan(
        routes_all, weights_all, plane, place, planes, group, seqs, slots
    )
    plane_out = share_columns(w_out, place, group, total)
    normed_in = rms_scale(tokens, mix_gain)
    q_proj = jnp.dot(normed_in, w_query, preferred_element_type=jnp.float32).astype(jnp.bfloat16)
    k_proj = jnp.dot(normed_in, w_key, preferred_element_type=jnp.float32).astype(jnp.bfloat16)
    v_proj = jnp.dot(normed_in, w_value, preferred_element_type=jnp.float32).astype(jnp.bfloat16)
    queries = rotate(q_proj.astype(jnp.float32).reshape(seqs, heads, head_k), positions)
    key_rows = rotate(
        k_proj.astype(jnp.float32).reshape(seqs, heads, head_k), positions
    ) * head_k ** (-0.5)
    values = v_proj.astype(jnp.float32).reshape(seqs, heads, head_v)
    decays = 1.0 - jnp.exp2(-2.0 - jnp.arange(heads, dtype=jnp.float32))
    new_state = (
        decays[None, :, None, None] * state + key_rows[:, :, :, None] * values[:, :, None, :]
    )
    readout = jnp.einsum("thd,thdv->thv", queries, new_state, precision=lax.Precision.HIGHEST)
    centre = jnp.mean(readout, axis=-1, keepdims=True)
    variance = jnp.mean(jnp.square(readout - centre), axis=-1, keepdims=True)
    normed = ((readout - centre) * lax.rsqrt(variance + EPS)).reshape(
        seqs, heads * head_v
    ) * ret_gain
    mixed = normed.astype(jnp.bfloat16)
    zsend = lambda x, s: lax.ppermute(x, "ep", [(d, (d + s * group) % total) for d in range(total)])
    mixed_pieces = [mixed] + [zsend(mixed, s) for s in range(1, planes)]
    mixed_all = jnp.concatenate(in_order(mixed_pieces, plane), axis=0)
    columns = lax.dot_general(
        mixed_all, plane_out, (((1,), (1,)), ((), ())), preferred_element_type=jnp.float32
    ).astype(jnp.bfloat16)
    column_pieces = [columns] + [zsend(columns, s) for s in range(1, planes)]
    attended = jnp.concatenate(in_order(column_pieces, plane), axis=1)
    resid = (tokens_all.astype(jnp.float32) + attended.astype(jnp.float32)).astype(jnp.bfloat16)
    normed_mid = rms_scale(resid, ffn_gain)
    outgoing = jnp.dot(dispatch, normed_mid, preferred_element_type=jnp.float32)
    outgoing = outgoing.astype(jnp.bfloat16).reshape(group, slots, width)
    swap = lambda x, s: lax.ppermute(x, "ep", [(d, d ^ s) for d in range(total)])
    arrivals = jnp.concatenate(
        [outgoing[0]] + [swap(outgoing[s], s) for s in range(1, group)], axis=0
    )
    gate_part = jnp.dot(arrivals, expert_gate[0], preferred_element_type=jnp.float32)
    up_part = jnp.dot(arrivals, expert_up[0], preferred_element_type=jnp.float32)
    hidden = (jax.nn.silu(gate_part) * up_part).astype(jnp.bfloat16)
    served = jnp.dot(hidden, expert_down[0], preferred_element_type=jnp.float32)
    served = served.astype(jnp.bfloat16).reshape(group, slots, width)
    returned = jnp.concatenate(
        [served[0]] + [swap(served[s], s) for s in range(1, group)], axis=0
    )
    parts = []
    for s in range(planes):
        block = lax.dynamic_index_in_dim(combine, (plane + s) % planes, 0, keepdims=False)
        both = jnp.dot(
            block.reshape(2 * seqs, group * slots), returned, preferred_element_type=jnp.float32
        )
        parts.append(both[:seqs] + both[seqs:])
    mixture = parts[0]
    for s in range(1, planes):
        mixture = mixture + zsend(parts[s].astype(jnp.bfloat16), s).astype(jnp.float32)
    own = lax.dynamic_slice_in_dim(resid, plane * seqs, seqs, 0)
    result = (own.astype(jnp.float32) + mixture).astype(jnp.bfloat16)
    return (result, new_state)


def solution(mesh):
    placed = (
        P("ep", None),
        P("ep"),
        P("ep", None, None, None),
        P(),
        P(),
        P(),
        P(),
        P(),
        P(None, "ep"),
        P(),
        P("ep", None),
        P("ep", None),
        P("ep", None, None),
        P("ep", None, None),
        P("ep", None, None),
    )
    return jax.shard_map(
        shards,
        mesh=mesh,
        in_specs=placed,
        out_specs=(P("ep", None), P("ep", None, None, None)),
        check_vma=False,
    )
```

```python
import math

import jax
import jax.numpy as jnp
from jax import lax
from jax.experimental.layout import Layout, with_layout_constraint
from jax.sharding import PartitionSpec as P

EPS = 1e-06


def rms_scale(values, gain):
    wide = values.astype(jnp.float32)
    scaled = wide * lax.rsqrt(jnp.mean(wide * wide, axis=-1, keepdims=True) + EPS)
    return (scaled * gain).astype(jnp.bfloat16)


def rotate(field, spots):
    half = field.shape[-1] // 2
    freqs = jnp.exp(-math.log(10000.0) * jnp.arange(half, dtype=jnp.float32) / half)
    angle = spots.astype(jnp.float32)[:, None] * freqs[None, :]
    cosine = jnp.cos(angle)[:, None, :]
    sine = jnp.sin(angle)[:, None, :]
    first = field[..., :half]
    second = field[..., half:]
    return jnp.concatenate(
        [first * cosine - second * sine, second * cosine + first * sine], axis=-1
    )


def send(values, pairs):
    flat = Layout(major_to_minor=tuple(range(values.ndim)))
    moved = lax.ppermute(with_layout_constraint(values, flat), "ep", pairs)
    return with_layout_constraint(moved, flat)


def in_order(pieces, turn):
    count = len(pieces)
    ordered = []
    for spot in range(count):
        chosen = pieces[0]
        for s in range(1, count):
            chosen = jnp.where((turn - spot) % count == s, pieces[s], chosen)
        ordered.append(chosen)
    return ordered


def share_tokens(tokens, routes, route_weights, plane, planes, group, total):
    width = tokens.shape[1]
    topk = routes.shape[1]
    high = route_weights.astype(jnp.bfloat16)
    low = (route_weights - high.astype(jnp.float32)).astype(jnp.bfloat16)
    extra = jnp.concatenate(
        [(routes // 256).astype(jnp.bfloat16), (routes % 256).astype(jnp.bfloat16), high, low],
        axis=1,
    )
    extra = jnp.pad(extra, ((0, 0), (0, -extra.shape[1] % 128)))
    packed = jnp.concatenate([tokens, extra], axis=1)
    pieces = [packed] + [
        send(packed, [(d, (d + s * group) % total) for d in range(total)])
        for s in range(1, planes)
    ]
    gathered = jnp.concatenate(in_order(pieces, plane), axis=0)
    small = gathered[:, width:].astype(jnp.float32)
    chosen = (small[:, :topk] * 256.0 + small[:, topk : 2 * topk]).astype(jnp.int32)
    halves = (small[:, 2 * topk : 3 * topk], small[:, 3 * topk : 4 * topk])
    return gathered[:, :width], chosen, halves


def plan(chosen, halves, plane, place, planes, group, seqs, slots):
    rows = chosen.shape[0]
    local = plane * group + (place ^ jnp.arange(group, dtype=jnp.int32))
    match = chosen[:, :, None] == local[None, None, :]
    hit = jnp.any(match, axis=1)
    high, low = (jnp.sum(jnp.where(match, half[:, :, None], 0.0), axis=1) for half in halves)
    before = jnp.arange(rows)[:, None] > jnp.arange(rows)[None, :]
    spot = jnp.dot(
        before.astype(jnp.bfloat16), hit.astype(jnp.bfloat16), preferred_element_type=jnp.float32
    ).astype(jnp.int32)
    spot = jnp.where(hit, spot, -1)
    one_hot = spot[:, :, None] == jnp.arange(slots, dtype=jnp.int32)[None, None, :]
    dispatch = jnp.transpose(one_hot, (1, 2, 0)).reshape(group * slots, rows).astype(jnp.bfloat16)
    combine = [
        jnp.where(one_hot, half[:, :, None], 0.0)
        .astype(jnp.bfloat16)
        .reshape(planes, seqs, group * slots)
        for half in (high, low)
    ]
    return dispatch, jnp.stack(combine, axis=1)


def share_columns(w_out, place, group, total):
    mine = w_out.T
    each = mine.shape[0]
    pieces = [mine] + [
        send(mine, [(d, d ^ s) for d in range(total)]) for s in range(1, group)
    ]
    spot = jnp.arange(group * each, dtype=jnp.int32)
    target = (place ^ (spot // each)) * each + spot % each
    order = (target[:, None] == spot[None, :]).astype(jnp.bfloat16)
    return jnp.concatenate(pieces, axis=0), order


def shards(
    tokens,
    positions,
    state,
    mix_gain,
    w_query,
    w_key,
    w_value,
    ret_gain,
    w_out,
    ffn_gain,
    routes,
    route_weights,
    expert_gate,
    expert_up,
    expert_down,
):
    seqs = tokens.shape[0]
    width = tokens.shape[1]
    heads = state.shape[1]
    head_k = state.shape[2]
    head_v = state.shape[3]
    total = lax.axis_size("ep")
    planes = 2 ** ((total.bit_length() - 1) // 2)
    group = total // planes
    index = lax.axis_index("ep")
    plane = index // group
    place = index % group
    topk = routes.shape[1]
    row_count = seqs * topk
    held = expert_gate.shape[0]
    experts = held * total
    capacity = max(2, 2 * row_count // experts) * planes
    slots = -(-capacity // 16) * 16
    tokens_all, routes_all, weights_all = share_tokens(
        tokens, routes, route_weights, plane, planes, group, total
    )
    dispatch, combine = plan(
        routes_all, weights_all, plane, place, planes, group, seqs, slots
    )
    plane_out, column_order = share_columns(w_out, place, group, total)
    normed_in = rms_scale(tokens, mix_gain)
    q_proj = jnp.dot(normed_in, w_query, preferred_element_type=jnp.float32).astype(jnp.bfloat16)
    k_proj = jnp.dot(normed_in, w_key, preferred_element_type=jnp.float32).astype(jnp.bfloat16)
    v_proj = jnp.dot(normed_in, w_value, preferred_element_type=jnp.float32).astype(jnp.bfloat16)
    queries = rotate(q_proj.astype(jnp.float32).reshape(seqs, heads, head_k), positions)
    key_rows = rotate(
        k_proj.astype(jnp.float32).reshape(seqs, heads, head_k), positions
    ) * head_k ** (-0.5)
    values = v_proj.astype(jnp.float32).reshape(seqs, heads, head_v)
    decays = 1.0 - jnp.exp2(-2.0 - jnp.arange(heads, dtype=jnp.float32))
    new_state = (
        decays[None, :, None, None] * state + key_rows[:, :, :, None] * values[:, :, None, :]
    )
    readout = jnp.einsum("thd,thdv->thv", queries, new_state, precision=lax.Precision.HIGHEST)
    centre = jnp.mean(readout, axis=-1, keepdims=True)
    variance = jnp.mean(jnp.square(readout - centre), axis=-1, keepdims=True)
    normed = ((readout - centre) * lax.rsqrt(variance + EPS)).reshape(
        seqs, heads * head_v
    ) * ret_gain
    mixed = normed.astype(jnp.bfloat16)
    zsend = lambda x, s: send(x, [(d, (d + s * group) % total) for d in range(total)])
    mixed_pieces = [mixed] + [zsend(mixed, s) for s in range(1, planes)]
    mixed_all = jnp.concatenate(in_order(mixed_pieces, plane), axis=0)
    columns = lax.dot_general(
        mixed_all, plane_out, (((1,), (1,)), ((), ())), preferred_element_type=jnp.float32
    ).astype(jnp.bfloat16)
    columns = jnp.dot(columns, column_order, preferred_element_type=jnp.float32).astype(jnp.bfloat16)
    column_pieces = [columns] + [zsend(columns, s) for s in range(1, planes)]
    attended = jnp.concatenate(in_order(column_pieces, plane), axis=1)
    resid = (tokens_all.astype(jnp.float32) + attended.astype(jnp.float32)).astype(jnp.bfloat16)
    normed_mid = rms_scale(resid, ffn_gain)
    outgoing = jnp.dot(dispatch, normed_mid, preferred_element_type=jnp.float32)
    outgoing = outgoing.astype(jnp.bfloat16).reshape(group, slots, width)
    swap = lambda x, s: send(x, [(d, d ^ s) for d in range(total)])
    arrivals = jnp.concatenate(
        [outgoing[0]] + [swap(outgoing[s], s) for s in range(1, group)], axis=0
    )
    gate_part = jnp.dot(arrivals, expert_gate[0], preferred_element_type=jnp.float32)
    up_part = jnp.dot(arrivals, expert_up[0], preferred_element_type=jnp.float32)
    hidden = (jax.nn.silu(gate_part) * up_part).astype(jnp.bfloat16)
    served = jnp.dot(hidden, expert_down[0], preferred_element_type=jnp.float32)
    served = served.astype(jnp.bfloat16).reshape(group, slots, width)
    returned = jnp.concatenate(
        [served[0]] + [swap(served[s], s) for s in range(1, group)], axis=0
    )
    parts = []
    for s in range(planes):
        block = lax.dynamic_index_in_dim(combine, (plane + s) % planes, 0, keepdims=False)
        both = jnp.dot(
            block.reshape(2 * seqs, group * slots), returned, preferred_element_type=jnp.float32
        )
        parts.append(both[:seqs] + both[seqs:])
    mixture = parts[0]
    for s in range(1, planes):
        mixture = mixture + zsend(parts[s].astype(jnp.bfloat16), s).astype(jnp.float32)
    own = lax.dynamic_slice_in_dim(resid, plane * seqs, seqs, 0)
    result = (own.astype(jnp.float32) + mixture).astype(jnp.bfloat16)
    return (result, new_state)


def solution(mesh):
    placed = (
        P("ep", None),
        P("ep"),
        P("ep", None, None, None),
        P(),
        P(),
        P(),
        P(),
        P(),
        P(None, "ep"),
        P(),
        P("ep", None),
        P("ep", None),
        P("ep", None, None),
        P("ep", None, None),
        P("ep", None, None),
    )
    return jax.shard_map(
        shards,
        mesh=mesh,
        in_specs=placed,
        out_specs=(P("ep", None), P("ep", None, None, None)),
        check_vma=False,
    )
```
